32 devices in a mesh: grp: 2 (over y), fs: 4 (over z), tp: 4 (over x, core).
Axes of the slice: x: 2, y: 2, z: 4, core: 2. Of those that a mesh axis runs over, the one named last changes fastest.
Arguments:
- inputs: bfloat16 [1024, 2048], P(('grp', 'fs'), 'tp'), parts along dimension 0, may hold values from -6 to 6
- mix_gain: float32 [2048], replicated, may hold values from 0.1 to 1.9
- query_weight: bfloat16 [2048, 1024], P('fs', 'tp'), may hold values from -0.125 to 0.125
- key_weight: bfloat16 [2048, 1024], P('fs', 'tp'), may hold values from -0.125 to 0.125
- value_weight: bfloat16 [2048, 2048], P('fs', 'tp'), may hold values from -0.125 to 0.125
- outgate_weight: bfloat16 [2048, 2048], P('fs', 'tp'), may hold values from -0.125 to 0.125
- decay_down: bfloat16 [2048, 32], replicated, may hold values from -0.125 to 0.125
- decay_up: bfloat16 [32, 1024], replicated, may hold values from -2 to 2
- decay_bias: float32 [1024], replicated, may hold values from -1 to 2
- head_gain: float32 [256], replicated, may hold values from 0.1 to 1.9
- mixout_weight: bfloat16 [2048, 2048], P('tp', 'fs'), may hold values from -0.125 to 0.125
- ffn_gain: float32 [2048], replicated, may hold values from 0.1 to 1.9
- upgate_weight: bfloat16 [2048, 4096], P('fs', 'tp'), may hold values from -0.125 to 0.125
- upvalue_weight: bfloat16 [2048, 4096], P('fs', 'tp'), may hold values from -0.125 to 0.125
- conv_gate: float32 [3, 4096], replicated, may hold values from -3.5 to 3.5
- conv_value: float32 [3, 4096], replicated, may hold values from -3.5 to 3.5
- down_weight: bfloat16 [4096, 2048], P('tp', 'fs'), may hold values from -0.09375 to 0.09375
Outputs:
- layer_out: bfloat16 [1024, 2048], P(('grp', 'fs'), 'tp'), parts along dimension 0
The draws below stay inside these ranges and needn't reach their ends.
There are 2 independent parts, one for each index of `grp`. The reference program is written for one: setup_inputs(seed, part) draws one part's arguments, and reference() takes and returns one part's arrays. A program takes and returns all parts, laid end to end along the dimension named above; an argument that names none is the same for every part. Nothing has to cross between parts.
All inputs are finite; a program needn't handle non-finite values.
Results may differ from the reference program's by a relative error of at most 0.018.
Values may be sent and summed in bfloat16 or wider, within the bound.
No kernel may reach another device: no remote copies, remote signals or barrier semaphores. Data moves between devices by JAX's collectives and lax.ppermute only.
A program may use at most 64 MiB of HBM per device.

```python
import jax
import jax.numpy as jnp
from jax import lax

D = 2048
HEADS = 8
DK = 128
DV = 256
RANK = 32
FF = 4096
BLOCK = 64
CONV = 3
TOK_DEV = 128
TOKENS = 512
KEY = 1024
VAL = 2048
N_TP = 4


def block_levels(own_key, shape, cuts, least, largest):
    loudness = 1.0
    for position, parts in cuts:
        steps = jax.random.uniform(jax.random.fold_in(jax.random.fold_in(own_key, 6), position), (parts,), jnp.float32, least / len(cuts), largest / len(cuts))
        loudness = loudness * jnp.repeat(jnp.exp(steps), shape[position] // parts).reshape((-1,) + (1,) * (len(shape) - 1 - position))
    return loudness


def noise(own_key, extent, spread, bound, cuts=(), held_as=jnp.bfloat16):
    level = block_levels(own_key, extent, cuts, -0.22, 0.18) if cuts else 1.0
    values = jax.random.normal(own_key, extent, jnp.float32) * spread * level
    return jnp.minimum(jnp.maximum(values, -bound), bound).astype(held_as)


def setup_inputs(seed: int = 0, part: int = 0) -> dict:
    key_of = jax.random.split(jax.random.key(seed), 18)
    part_keys = jax.random.split(jax.random.fold_in(key_of[17], part), 18)
    return {
        "inputs": noise(part_keys[0], (TOKENS, D), 1.0, 6.0, ((0, 4), (1, 4))),
        "mix_gain": jnp.clip(1.0 + 0.18 * jax.random.normal(key_of[1], (D,), jnp.float32), 0.1, 1.9),
        "query_weight": noise(key_of[2], (D, KEY), D ** -0.5, 0.125, ((0, 4), (1, 4))),
        "key_weight": noise(key_of[3], (D, KEY), D ** -0.5, 0.125, ((0, 4), (1, 4))),
        "value_weight": noise(key_of[4], (D, VAL), D ** -0.5, 0.125, ((0, 4), (1, 4))),
        "outgate_weight": noise(key_of[5], (D, VAL), D ** -0.5, 0.125, ((0, 4), (1, 4))),
        "decay_down": noise(key_of[6], (D, RANK), D ** -0.5, 0.125),
        "decay_up": noise(key_of[7], (RANK, KEY), (RANK // 4) ** -0.5, 2.0),
        "decay_bias": jnp.clip(jax.random.uniform(key_of[8], (KEY,), jnp.float32, -1.0, 2.0), -1.0, 2.0),
        "head_gain": jnp.clip(1.0 + 0.18 * jax.random.normal(key_of[9], (DV,), jnp.float32), 0.1, 1.9),
        "mixout_weight": noise(key_of[10], (VAL, D), VAL ** -0.5, 0.125, ((0, 4), (1, 4))),
        "ffn_gain": jnp.clip(1.0 + 0.18 * jax.random.normal(key_of[11], (D,), jnp.float32), 0.1, 1.9),
        "upgate_weight": noise(key_of[12], (D, FF), D ** -0.5, 0.125, ((0, 4), (1, 4))),
        "upvalue_weight": noise(key_of[13], (D, FF), D ** -0.5, 0.125, ((0, 4), (1, 4))),
        "conv_gate": noise(key_of[14], (CONV, FF), CONV ** -0.5, 3.5, (), jnp.float32),
        "conv_value": noise(key_of[15], (CONV, FF), CONV ** -0.5, 3.5, (), jnp.float32),
        "down_weight": noise(key_of[16], (FF, D), FF ** -0.5, 0.09375, ((0, 4), (1, 4))),
    }


EPS = 1e-06
GATE_NORM = 16.0
HIGH = lax.Precision.HIGHEST

def product(left, right):
    return jnp.dot(left, right, preferred_element_type=jnp.float32)

def root_norm(values, gain):
    return values * lax.rsqrt(lax.optimization_barrier(jnp.mean(values * values, axis=-1, keepdims=True)) + EPS) * gain

def linear_attention(queries, key_rows, value_rows, log_decay):
    count, length, heads, key_size = queries.shape
    blocks = length // BLOCK

    def split(tensor):
        return tensor.astype(jnp.float32).reshape(count, blocks, BLOCK, heads, -1).transpose(0, 3, 1, 2, 4)
    scaled = split(queries) * key_size ** (-0.5)
    keyed = split(key_rows)
    valued = split(value_rows)
    running = jnp.cumsum(split(log_decay), axis=3)
    final = running[:, :, :, -1:]
    query_in = scaled * jnp.exp(running)
    key_in = keyed * jnp.exp(-running)
    key_end = keyed * jnp.exp(final - running)
    causal = jnp.tril(jnp.ones((BLOCK, BLOCK), dtype=bool))
    scores = jnp.einsum('shnik,shnjk->shnij', query_in, key_in, precision=HIGH)
    scores = jnp.where(causal, scores, 0.0)
    inside = jnp.einsum('shnij,shnjv->shniv', scores, valued, precision=HIGH)
    update = jnp.einsum('shnck,shncv->shnkv', key_end, valued, precision=HIGH)
    factor = jnp.exp(final[:, :, :, 0])

    def advance(state, pair):
        return (pair[0][..., None] * state + pair[1], state)
    initial = jnp.zeros((count, heads, key_size, valued.shape[-1]), jnp.float32)
    _, starts = lax.scan(advance, initial, (jnp.moveaxis(factor, 2, 0), jnp.moveaxis(update, 2, 0)))
    starts = jnp.moveaxis(starts, 0, 2)
    carried = jnp.einsum('shnck,shnkv->shncv', query_in, starts, precision=HIGH)
    merged = inside + carried
    return merged.transpose(0, 2, 3, 1, 4).reshape(count, length, heads * valued.shape[-1])

def causal_conv(rows, taps, length):
    channels = rows.shape[-1]
    shaped = rows.astype(jnp.float32).reshape(-1, length, channels)
    padded = jnp.pad(shaped, ((0, 0), (CONV - 1, 0), (0, 0)))
    total = jnp.zeros_like(shaped)
    for offset in range(CONV):
        total = total + padded[:, offset:offset + length] * taps[offset]
    return total.reshape(-1, channels)

def grouped(left, weight):
    width = weight.shape[0] // N_TP
    total = jnp.zeros((left.shape[0], weight.shape[1]), jnp.float32)
    for member in range(N_TP):
        term = product(left[:, member * width:(member + 1) * width], weight[member * width:(member + 1) * width]).astype(jnp.bfloat16)
        total = total + lax.optimization_barrier(term).astype(jnp.float32)
    return total

def reference(inputs, mix_gain, query_weight, key_weight, value_weight, outgate_weight, decay_down, decay_up, decay_bias, head_gain, mixout_weight, ffn_gain, upgate_weight, upvalue_weight, conv_gate, conv_value, down_weight):
    count = TOKENS // TOK_DEV
    normed_mix = root_norm(inputs.astype(jnp.float32), mix_gain).astype(jnp.bfloat16)
    queries = product(normed_mix, query_weight).astype(jnp.bfloat16)
    key_rows = product(normed_mix, key_weight).astype(jnp.bfloat16)
    value_rows = product(normed_mix, value_weight).astype(jnp.bfloat16)
    out_gates = product(normed_mix, outgate_weight).astype(jnp.bfloat16)
    decay_low = product(normed_mix, decay_down).astype(jnp.bfloat16)
    log_decay = jax.nn.log_sigmoid(product(decay_low, decay_up) + decay_bias) / GATE_NORM
    attended = linear_attention(queries.reshape(count, TOK_DEV, HEADS, DK), key_rows.reshape(count, TOK_DEV, HEADS, DK), value_rows.reshape(count, TOK_DEV, HEADS, DV), log_decay.reshape(count, TOK_DEV, HEADS, DK))
    attended = attended.reshape(TOKENS, HEADS, DV)
    gated = root_norm(attended, head_gain) * jax.nn.silu(out_gates.astype(jnp.float32).reshape(TOKENS, HEADS, DV))
    gated = gated.reshape(TOKENS, VAL).astype(jnp.bfloat16)
    mixed = grouped(gated, mixout_weight)
    stream = (inputs.astype(jnp.float32) + mixed).astype(jnp.bfloat16)
    normed_ffn = root_norm(stream.astype(jnp.float32), ffn_gain).astype(jnp.bfloat16)
    up_gates = product(normed_ffn, upgate_weight).astype(jnp.bfloat16)
    up_values = product(normed_ffn, upvalue_weight).astype(jnp.bfloat16)
    conv_gates = causal_conv(up_gates, conv_gate, TOK_DEV)
    conv_values = causal_conv(up_values, conv_value, TOK_DEV)
    hidden = (jax.nn.gelu(conv_gates, approximate=True) * conv_values).astype(jnp.bfloat16)
    channel_sums = grouped(hidden, down_weight)
    return (stream.astype(jnp.float32) + channel_sums).astype(jnp.bfloat16)
```

```python
import functools

import jax
import jax.numpy as jnp
from jax import lax
from jax.experimental import pallas as pl
from jax.experimental.pallas import tpu as pltpu
from jax.sharding import PartitionSpec as P

DK = 128
DV = 256
BLOCK = 64
CONV = 3


EPS = 1e-06
GATE_NORM = 16.0
HIGH = lax.Precision.HIGHEST


def product(left, right):
    return jnp.dot(left, right, preferred_element_type=jnp.float32)


def root_norm(values, gain):
    return values * lax.rsqrt(jnp.mean(values * values, axis=-1, keepdims=True) + EPS) * gain


def linear_attention(queries, key_rows, value_rows, log_decay):
    count, length, heads, key_size = queries.shape
    blocks = length // BLOCK

    def split(tensor):
        return (
            tensor.astype(jnp.float32)
            .reshape(count, blocks, BLOCK, heads, -1)
            .transpose(0, 3, 1, 2, 4)
        )

    scaled = split(queries) * key_size ** (-0.5)
    keyed = split(key_rows)
    valued = split(value_rows)
    running = jnp.cumsum(split(log_decay), axis=3)
    final = running[:, :, :, -1:]
    query_in = scaled * jnp.exp(running)
    key_in = keyed * jnp.exp(-running)
    key_end = keyed * jnp.exp(final - running)
    causal = jnp.tril(jnp.ones((BLOCK, BLOCK), dtype=bool))
    scores = jnp.einsum("shnik,shnjk->shnij", query_in, key_in, precision=HIGH)
    scores = jnp.where(causal, scores, 0.0)
    inside = jnp.einsum("shnij,shnjv->shniv", scores, valued, precision=HIGH)
    update = jnp.einsum("shnck,shncv->shnkv", key_end, valued, precision=HIGH)
    factor = jnp.exp(final[:, :, :, 0])

    def advance(state, pair):
        return (pair[0][..., None] * state + pair[1], state)

    initial = jnp.zeros((count, heads, key_size, valued.shape[-1]), jnp.float32)
    _, starts = lax.scan(advance, initial, (jnp.moveaxis(factor, 2, 0), jnp.moveaxis(update, 2, 0)))
    starts = jnp.moveaxis(starts, 0, 2)
    carried = jnp.einsum("shnck,shnkv->shncv", query_in, starts, precision=HIGH)
    merged = inside + carried
    return merged.transpose(0, 2, 3, 1, 4).reshape(count, length, heads * valued.shape[-1])


def causal_conv(rows, taps):
    length = rows.shape[0]
    padded = jnp.pad(rows.astype(jnp.float32), ((CONV - 1, 0), (0, 0)))
    total = jnp.zeros((length, rows.shape[1]), jnp.float32)
    for offset in range(CONV):
        total = total + padded[offset : offset + length] * taps[offset]
    return total


def per_device(
    inputs,
    mix_gain,
    query_weight,
    key_weight,
    value_weight,
    outgate_weight,
    decay_down,
    decay_up,
    decay_bias,
    head_gain,
    mixout_weight,
    ffn_gain,
    upgate_weight,
    upvalue_weight,
    conv_gate,
    conv_value,
    down_weight,
):
    position = lax.axis_index("tp")
    whole = lax.all_gather(inputs, "tp", axis=1, tiled=True)
    normed_mix = root_norm(whole.astype(jnp.float32), mix_gain).astype(jnp.bfloat16)
    length = normed_mix.shape[0]
    key_cols = query_weight.shape[1]
    value_cols = value_weight.shape[1]
    local_heads = key_cols // DK
    pieces = (
        lax.all_gather(query_weight, "fs", axis=0, tiled=True),
        lax.all_gather(key_weight, "fs", axis=0, tiled=True),
        lax.all_gather(value_weight, "fs", axis=0, tiled=True),
        lax.all_gather(outgate_weight, "fs", axis=0, tiled=True),
    )
    queries, key_rows, value_rows, out_gates = tuple(
        (product(normed_mix, piece) for piece in pieces)
    )
    queries = queries.astype(jnp.bfloat16)
    key_rows = key_rows.astype(jnp.bfloat16)
    value_rows = value_rows.astype(jnp.bfloat16)
    out_gates = out_gates.astype(jnp.bfloat16)
    decay_low = product(normed_mix, decay_down).astype(jnp.bfloat16)
    own_up = lax.dynamic_slice_in_dim(decay_up, position * key_cols, key_cols, 1)
    own_bias = lax.dynamic_slice_in_dim(decay_bias, position * key_cols, key_cols, 0)
    log_decay = jax.nn.log_sigmoid(product(decay_low, own_up) + own_bias) / GATE_NORM
    attended = linear_attention(
        queries.reshape(1, length, local_heads, DK),
        key_rows.reshape(1, length, local_heads, DK),
        value_rows.reshape(1, length, local_heads, DV),
        log_decay.reshape(1, length, local_heads, DK),
    )
    attended = attended.reshape(length, local_heads, DV)
    gated = root_norm(attended, head_gain) * jax.nn.silu(
        out_gates.astype(jnp.float32).reshape(length, local_heads, DV)
    )
    gated = gated.reshape(length, value_cols).astype(jnp.bfloat16)
    mix_terms = product(gated, lax.all_gather(mixout_weight, "fs", axis=1, tiled=True))
    mixed = lax.psum_scatter(
        mix_terms.astype(jnp.bfloat16), "tp", scatter_dimension=1, tiled=True
    ).astype(jnp.float32)
    stream = (inputs.astype(jnp.float32) + mixed).astype(jnp.bfloat16)
    whole_stream = lax.all_gather(stream, "tp", axis=1, tiled=True)
    normed_ffn = root_norm(whole_stream.astype(jnp.float32), ffn_gain).astype(jnp.bfloat16)
    hidden_cols = upgate_weight.shape[1]
    gate_full, value_full = (
        lax.all_gather(upgate_weight, "fs", axis=0, tiled=True),
        lax.all_gather(upvalue_weight, "fs", axis=0, tiled=True),
    )
    up_gates = product(normed_ffn, gate_full)
    up_values = product(normed_ffn, value_full)
    up_gates = up_gates.astype(jnp.bfloat16)
    up_values = up_values.astype(jnp.bfloat16)
    taps_gate = lax.dynamic_slice_in_dim(conv_gate, position * hidden_cols, hidden_cols, 1)
    taps_value = lax.dynamic_slice_in_dim(conv_value, position * hidden_cols, hidden_cols, 1)
    conv_gates = causal_conv(up_gates, taps_gate)
    conv_values = causal_conv(up_values, taps_value)
    hidden = (jax.nn.gelu(conv_gates, approximate=True) * conv_values).astype(jnp.bfloat16)
    down_terms = product(hidden, lax.all_gather(down_weight, "fs", axis=1, tiled=True))
    channel_sums = lax.psum_scatter(
        down_terms.astype(jnp.bfloat16), "tp", scatter_dimension=1, tiled=True
    ).astype(jnp.float32)
    return (stream.astype(jnp.float32) + channel_sums).astype(jnp.bfloat16)


LANES = 128


def cost(flops, moved):
    return pl.CostEstimate(flops=flops, bytes_accessed=moved, transcendentals=0)


def slot(shift, size):
    wide = jnp.int32(shift) % size
    return jnp.where(wide < 0, wide + size, wide)


def project_kernel(scalars, *refs, size, extra_rank):
    chunks = refs[:size]
    gain = refs[size]
    outs = refs[-size - 1 : -1]
    scratch = refs[-1]
    weights = refs[size + 1 : -size - 1]
    extra = weights[-1] if extra_rank else None
    weights = weights[:-1] if extra_rank else weights
    width = sum(weight.shape[1] for weight in weights)
    rows = chunks[0].shape[0]
    lane = lax.broadcasted_iota(jnp.int32, (rows, LANES), 1)
    for index, chunk in enumerate(chunks):
        values = chunk[...].astype(jnp.float32)
        total = jnp.sum(values * values, axis=1, keepdims=True)
        scaled = (values * gain[...]).astype(jnp.bfloat16)
        if extra_rank:
            side = product(scaled, extra[...])
        else:
            side = jnp.zeros((rows, LANES), jnp.float32)
        high = total.astype(jnp.bfloat16).astype(jnp.float32)
        side = jnp.where(lane == extra_rank, high, side)
        side = jnp.where(lane == extra_rank + 1, total - high, side)
        scratch[scalars[index], :, : values.shape[1]] = scaled
        scratch[scalars[index], :, values.shape[1] :] = side.astype(jnp.bfloat16)
    inner = chunks[0].shape[1]
    for index, out in enumerate(outs):
        left = scratch[index, :, :inner]
        start = 0
        for weight in weights:
            stop = start + weight.shape[1]
            out[:, start:stop] = product(left, weight[...]).astype(jnp.bfloat16)
            start = stop
        out[:, width:] = scratch[index, :, inner:]


def project(chunks, order, gain, weights, extra, extra_rank):
    size = len(chunks)
    rows, inner = chunks[0].shape
    width = sum(weight.shape[1] for weight in weights) + LANES
    operands = [*chunks, gain.reshape(1, -1), *weights] + ([extra] if extra_rank else [])
    return pl.pallas_call(
        functools.partial(project_kernel, size=size, extra_rank=extra_rank),
        out_shape=[jax.ShapeDtypeStruct((rows, width), jnp.bfloat16)] * size,
        in_specs=[pl.BlockSpec(memory_space=pltpu.SMEM)]
        + [pl.BlockSpec(memory_space=pltpu.VMEM)] * len(operands),
        out_specs=[pl.BlockSpec(memory_space=pltpu.VMEM)] * size,
        scratch_shapes=[pltpu.VMEM((size, rows, inner + LANES), jnp.bfloat16)],
        cost_estimate=cost(2 * size * rows * inner * width, 2 * inner * width),
        name="project",
    )(order, *operands)


def spread_kernel(scalars, *refs, size):
    chunks = refs[:size]
    weight = refs[size]
    outs = refs[size + 1 : -1]
    scratch = refs[-1]
    for index, chunk in enumerate(chunks):
        scratch[scalars[index]] = chunk[...]
    for index, out in enumerate(outs):
        out[...] = product(scratch[index], weight[...]).astype(jnp.bfloat16)


def spread(chunks, order, weight):
    size = len(chunks)
    rows, inner = chunks[0].shape
    width = weight.shape[1]
    return pl.pallas_call(
        functools.partial(spread_kernel, size=size),
        out_shape=[jax.ShapeDtypeStruct((rows, width), jnp.bfloat16)] * size,
        in_specs=[pl.BlockSpec(memory_space=pltpu.SMEM)]
        + [pl.BlockSpec(memory_space=pltpu.VMEM)] * (size + 1),
        out_specs=[pl.BlockSpec(memory_space=pltpu.VMEM)] * size,
        scratch_shapes=[pltpu.VMEM((size, rows, inner), jnp.bfloat16)],
        cost_estimate=cost(2 * size * rows * inner * width, 2 * inner * width),
        name="spread",
    )(order, *chunks, weight)


def total_of(terms, start, stop):
    total = terms[0][:, start:stop].astype(jnp.float32)
    for term in terms[1:]:
        total = total + term[:, start:stop].astype(jnp.float32)
    return total


def inverse_root(side, extra_rank, features):
    squares = side[:, extra_rank : extra_rank + 1] + side[:, extra_rank + 1 : extra_rank + 2]
    return lax.rsqrt(squares / features + EPS)


def exact(left, right, dims):
    return lax.dot_general(
        left, right, (dims, ((), ())), precision=HIGH, preferred_element_type=jnp.float32
    )


def attend_kernel(*refs, size, key_cols, value_cols, rank, features):
    terms = refs[:size]
    decay_up, decay_bias, head_gain, out, attended_ref = refs[size:]
    width = 2 * key_cols + 2 * value_cols
    side = total_of(terms, width, width + LANES)
    scale = inverse_root(side, rank, features)
    lane = lax.broadcasted_iota(jnp.int32, side.shape, 1)
    low = jnp.where(lane < rank, side * scale, 0.0).astype(jnp.bfloat16)
    decay = jax.nn.log_sigmoid(product(low, decay_up[...]) + decay_bias[...]) / GATE_NORM
    length = side.shape[0]
    row = lax.broadcasted_iota(jnp.int32, (BLOCK, BLOCK), 0)
    column = lax.broadcasted_iota(jnp.int32, (BLOCK, BLOCK), 1)
    causal = row >= column
    lower = jnp.where(causal, 1.0, 0.0)

    def piece(start, stop):
        rounded = (total_of(terms, start, stop) * scale).astype(jnp.bfloat16)
        return rounded.astype(jnp.float32)

    queries = piece(0, key_cols) * DK ** (-0.5)
    key_rows = piece(key_cols, 2 * key_cols)
    value_rows = piece(2 * key_cols, 2 * key_cols + value_cols)
    gates = piece(2 * key_cols + value_cols, width)
    gates = gates / (1.0 + jnp.exp(-gates))
    for head in range(key_cols // DK):
        keys = slice(head * DK, (head + 1) * DK)
        values = slice(head * DV, (head + 1) * DV)
        state = None
        for block in range(length // BLOCK):
            here = slice(block * BLOCK, (block + 1) * BLOCK)
            running = exact(lower, decay[here, keys], ((1,), (0,)))
            final = running[BLOCK - 1 : BLOCK]
            query_in = queries[here, keys] * jnp.exp(running)
            keyed = key_rows[here, keys]
            valued = value_rows[here, values]
            scores = exact(query_in, keyed * jnp.exp(-running), ((1,), (1,)))
            scores = jnp.where(causal, scores, 0.0)
            attended = exact(scores, valued, ((1,), (0,)))
            if state is not None:
                attended = attended + exact(query_in, state, ((1,), (0,)))
            attended_ref[here, values] = attended
            if block + 1 < length // BLOCK:
                key_end = keyed * jnp.exp(final - running)
                update = exact(key_end, valued, ((0,), (0,)))
                factor = jnp.exp(final).reshape(DK, 1)
                state = update if state is None else factor * state + update
        heads = attended_ref[:, values]
        normed = root_norm(heads, head_gain[...])
        out[:, values] = (normed * gates[:, values]).astype(jnp.bfloat16)


def attend(terms, decay_up, decay_bias, head_gain, key_cols, value_cols, rank, features):
    rows = terms[0].shape[0]
    return pl.pallas_call(
        functools.partial(
            attend_kernel,
            size=len(terms),
            key_cols=key_cols,
            value_cols=value_cols,
            rank=rank,
            features=features,
        ),
        out_shape=jax.ShapeDtypeStruct((rows, value_cols), jnp.bfloat16),
        scratch_shapes=[pltpu.VMEM((rows, value_cols), jnp.float32)],
        name="attend",
    )(*terms, decay_up, decay_bias.reshape(1, -1), head_gain.reshape(1, -1))


def hidden_kernel(*refs, size, hidden_cols, features):
    terms = refs[:size]
    taps_gate, taps_value, out = refs[size:]
    side = total_of(terms, 2 * hidden_cols, 2 * hidden_cols + LANES)
    scale = inverse_root(side, 0, features)
    step = 2 * LANES if hidden_cols % (2 * LANES) == 0 else hidden_cols

    def conv(start, taps):
        rows = (total_of(terms, start, start + step) * scale).astype(jnp.bfloat16)
        rows = rows.astype(jnp.float32)
        position = lax.broadcasted_iota(jnp.int32, rows.shape, 0)
        total = jnp.zeros_like(rows)
        for offset in range(CONV):
            back = CONV - 1 - offset
            moved = pltpu.roll(rows, back, 0) if back else rows
            moved = jnp.where(position >= back, moved, 0.0)
            total = total + moved * taps[offset : offset + 1]
        return total

    for start in range(0, hidden_cols, step):
        cols = slice(start, start + step)
        gates = conv(start, taps_gate[:, cols])
        values = conv(hidden_cols + start, taps_value[:, cols])
        out[:, cols] = (jax.nn.gelu(gates, approximate=True) * values).astype(jnp.bfloat16)


def hidden_units(terms, taps_gate, taps_value, features):
    rows = terms[0].shape[0]
    hidden_cols = taps_gate.shape[1]
    return pl.pallas_call(
        functools.partial(
            hidden_kernel, size=len(terms), hidden_cols=hidden_cols, features=features
        ),
        out_shape=jax.ShapeDtypeStruct((rows, hidden_cols), jnp.bfloat16),
        name="hidden",
    )(*terms, taps_gate, taps_value)


def moving_activations(
    inputs,
    mix_gain,
    query_weight,
    key_weight,
    value_weight,
    outgate_weight,
    decay_down,
    decay_up,
    decay_bias,
    head_gain,
    mixout_weight,
    ffn_gain,
    upgate_weight,
    upvalue_weight,
    conv_gate,
    conv_value,
    down_weight,
    *,
    size,
):
    line = lax.axis_index("fs")
    position = lax.axis_index("tp")
    features = mix_gain.shape[0]
    own = query_weight.shape[0]
    key_cols = query_weight.shape[1]
    value_cols = value_weight.shape[1]
    hidden_cols = upgate_weight.shape[1]
    rank = decay_down.shape[1]
    steps = range(size)
    both = ("fs", "tp")

    def along(axis, shift, array):
        if shift == 0:
            return array
        return lax.ppermute(array, axis, [(at, (at + shift) % size) for at in steps])

    def crossed(shift, array, turned):
        pairs = []
        for a in steps:
            for b in steps:
                there = ((b + shift) % size, a) if turned else (b, (a + shift) % size)
                pairs.append((a * size + b, there[0] * size + there[1]))
        return lax.ppermute(array, both, pairs)

    def order(base):
        return jnp.stack([slot(base - shift, size) for shift in steps])

    def summed(terms):
        total = terms[0].astype(jnp.float32)
        for term in terms[1:]:
            total = total + term.astype(jnp.float32)
        return total

    own_gain = lax.dynamic_slice_in_dim(mix_gain, line * own, own, 0)
    own_ffn = lax.dynamic_slice_in_dim(ffn_gain, line * own, own, 0)
    own_down = lax.dynamic_slice_in_dim(decay_down, line * own, own, 0)
    own_down = jnp.pad(own_down, ((0, 0), (0, LANES - rank)))
    own_up = lax.dynamic_slice_in_dim(decay_up, position * key_cols, key_cols, 1)
    own_up = jnp.pad(own_up, ((0, LANES - rank), (0, 0)))
    own_bias = lax.dynamic_slice_in_dim(decay_bias, position * key_cols, key_cols, 0)
    taps_gate = lax.dynamic_slice_in_dim(conv_gate, position * hidden_cols, hidden_cols, 1)
    taps_value = lax.dynamic_slice_in_dim(conv_value, position * hidden_cols, hidden_cols, 1)

    chunks = [crossed(shift, inputs, False) for shift in steps]
    parts = project(
        chunks,
        order(position - line),
        own_gain,
        (query_weight, key_weight, value_weight, outgate_weight),
        own_down,
        rank,
    )
    terms = [along("fs", shift, parts[shift]) for shift in steps]
    gated = attend(terms, own_up, own_bias, head_gain, key_cols, value_cols, rank, features)

    rows = [along("fs", shift, gated) for shift in steps]
    parts = spread(rows, order(line - position), mixout_weight)
    mixed = summed([along("tp", shift, parts[shift]) for shift in steps])
    stream = (chunks[0].astype(jnp.float32) + mixed).astype(jnp.bfloat16)
    streams = [along("tp", shift, stream) for shift in steps]
    own_stream = crossed(0, stream, False)
    parts = project(
        streams, order(position - line), own_ffn, (upgate_weight, upvalue_weight), None, 0
    )
    terms = [along("fs", shift, parts[shift]) for shift in steps]
    hidden = hidden_units(terms, taps_gate, taps_value, features)

    rows = [along("fs", shift, hidden) for shift in steps]
    parts = spread(rows, order(line - position), down_weight)
    channel_sums = summed([crossed(shift, parts[shift], True) for shift in steps])
    return (own_stream.astype(jnp.float32) + channel_sums).astype(jnp.bfloat16)


def solution(mesh):
    plan = per_device
    if mesh.shape["fs"] == mesh.shape["tp"]:
        plan = functools.partial(moving_activations, size=mesh.shape["fs"])
    return jax.shard_map(
        plan,
        mesh=mesh,
        in_specs=(
            P(("grp", "fs"), "tp"),
            P(),
            P("fs", "tp"),
            P("fs", "tp"),
            P("fs", "tp"),
            P("fs", "tp"),
            P(),
            P(),
            P(),
            P(),
            P("tp", "fs"),
            P(),
            P("fs", "tp"),
            P("fs", "tp"),
            P(),
            P(),
            P("tp", "fs"),
        ),
        out_specs=P(("grp", "fs"), "tp"),
        check_vma=False,
    )
```

```python
import functools

import jax
import jax.numpy as jnp
from jax import lax
from jax.experimental import pallas as pl
from jax.experimental.pallas import tpu as pltpu
from jax.sharding import PartitionSpec as P

DK = 128
DV = 256
BLOCK = 64
CONV = 3


EPS = 1e-06
GATE_NORM = 16.0
HIGH = lax.Precision.HIGHEST


def product(left, right):
    return jnp.dot(left, right, preferred_element_type=jnp.float32)


def root_norm(values, gain):
    return values * lax.rsqrt(jnp.mean(values * values, axis=-1, keepdims=True) + EPS) * gain


def linear_attention(queries, key_rows, value_rows, log_decay):
    count, length, heads, key_size = queries.shape
    blocks = length // BLOCK

    def split(tensor):
        return (
            tensor.astype(jnp.float32)
            .reshape(count, blocks, BLOCK, heads, -1)
            .transpose(0, 3, 1, 2, 4)
        )

    scaled = split(queries) * key_size ** (-0.5)
    keyed = split(key_rows)
    valued = split(value_rows)
    running = jnp.cumsum(split(log_decay), axis=3)
    final = running[:, :, :, -1:]
    query_in = scaled * jnp.exp(running)
    key_in = keyed * jnp.exp(-running)
    key_end = keyed * jnp.exp(final - running)
    causal = jnp.tril(jnp.ones((BLOCK, BLOCK), dtype=bool))
    scores = jnp.einsum("shnik,shnjk->shnij", query_in, key_in, precision=HIGH)
    scores = jnp.where(causal, scores, 0.0)
    inside = jnp.einsum("shnij,shnjv->shniv", scores, valued, precision=HIGH)
    update = jnp.einsum("shnck,shncv->shnkv", key_end, valued, precision=HIGH)
    factor = jnp.exp(final[:, :, :, 0])

    def advance(state, pair):
        return (pair[0][..., None] * state + pair[1], state)

    initial = jnp.zeros((count, heads, key_size, valued.shape[-1]), jnp.float32)
    _, starts = lax.scan(advance, initial, (jnp.moveaxis(factor, 2, 0), jnp.moveaxis(update, 2, 0)))
    starts = jnp.moveaxis(starts, 0, 2)
    carried = jnp.einsum("shnck,shnkv->shncv", query_in, starts, precision=HIGH)
    merged = inside + carried
    return merged.transpose(0, 2, 3, 1, 4).reshape(count, length, heads * valued.shape[-1])


def causal_conv(rows, taps):
    length = rows.shape[0]
    padded = jnp.pad(rows.astype(jnp.float32), ((CONV - 1, 0), (0, 0)))
    total = jnp.zeros((length, rows.shape[1]), jnp.float32)
    for offset in range(CONV):
        total = total + padded[offset : offset + length] * taps[offset]
    return total


def per_device(
    inputs,
    mix_gain,
    query_weight,
    key_weight,
    value_weight,
    outgate_weight,
    decay_down,
    decay_up,
    decay_bias,
    head_gain,
    mixout_weight,
    ffn_gain,
    upgate_weight,
    upvalue_weight,
    conv_gate,
    conv_value,
    down_weight,
):
    position = lax.axis_index("tp")
    whole = lax.all_gather(inputs, "tp", axis=1, tiled=True)
    normed_mix = root_norm(whole.astype(jnp.float32), mix_gain).astype(jnp.bfloat16)
    length = normed_mix.shape[0]
    key_cols = query_weight.shape[1]
    value_cols = value_weight.shape[1]
    local_heads = key_cols // DK
    pieces = (
        lax.all_gather(query_weight, "fs", axis=0, tiled=True),
        lax.all_gather(key_weight, "fs", axis=0, tiled=True),
        lax.all_gather(value_weight, "fs", axis=0, tiled=True),
        lax.all_gather(outgate_weight, "fs", axis=0, tiled=True),
    )
    queries, key_rows, value_rows, out_gates = tuple(
        (product(normed_mix, piece) for piece in pieces)
    )
    queries = queries.astype(jnp.bfloat16)
    key_rows = key_rows.astype(jnp.bfloat16)
    value_rows = value_rows.astype(jnp.bfloat16)
    out_gates = out_gates.astype(jnp.bfloat16)
    decay_low = product(normed_mix, decay_down).astype(jnp.bfloat16)
    own_up = lax.dynamic_slice_in_dim(decay_up, position * key_cols, key_cols, 1)
    own_bias = lax.dynamic_slice_in_dim(decay_bias, position * key_cols, key_cols, 0)
    log_decay = jax.nn.log_sigmoid(product(decay_low, own_up) + own_bias) / GATE_NORM
    attended = linear_attention(
        queries.reshape(1, length, local_heads, DK),
        key_rows.reshape(1, length, local_heads, DK),
        value_rows.reshape(1, length, local_heads, DV),
        log_decay.reshape(1, length, local_heads, DK),
    )
    attended = attended.reshape(length, local_heads, DV)
    gated = root_norm(attended, head_gain) * jax.nn.silu(
        out_gates.astype(jnp.float32).reshape(length, local_heads, DV)
    )
    gated = gated.reshape(length, value_cols).astype(jnp.bfloat16)
    mix_terms = product(gated, lax.all_gather(mixout_weight, "fs", axis=1, tiled=True))
    mixed = lax.psum_scatter(
        mix_terms.astype(jnp.bfloat16), "tp", scatter_dimension=1, tiled=True
    ).astype(jnp.float32)
    stream = (inputs.astype(jnp.float32) + mixed).astype(jnp.bfloat16)
    whole_stream = lax.all_gather(stream, "tp", axis=1, tiled=True)
    normed_ffn = root_norm(whole_stream.astype(jnp.float32), ffn_gain).astype(jnp.bfloat16)
    hidden_cols = upgate_weight.shape[1]
    gate_full, value_full = (
        lax.all_gather(upgate_weight, "fs", axis=0, tiled=True),
        lax.all_gather(upvalue_weight, "fs", axis=0, tiled=True),
    )
    up_gates = product(normed_ffn, gate_full)
    up_values = product(normed_ffn, value_full)
    up_gates = up_gates.astype(jnp.bfloat16)
    up_values = up_values.astype(jnp.bfloat16)
    taps_gate = lax.dynamic_slice_in_dim(conv_gate, position * hidden_cols, hidden_cols, 1)
    taps_value = lax.dynamic_slice_in_dim(conv_value, position * hidden_cols, hidden_cols, 1)
    conv_gates = causal_conv(up_gates, taps_gate)
    conv_values = causal_conv(up_values, taps_value)
    hidden = (jax.nn.gelu(conv_gates, approximate=True) * conv_values).astype(jnp.bfloat16)
    down_terms = product(hidden, lax.all_gather(down_weight, "fs", axis=1, tiled=True))
    channel_sums = lax.psum_scatter(
        down_terms.astype(jnp.bfloat16), "tp", scatter_dimension=1, tiled=True
    ).astype(jnp.float32)
    return (stream.astype(jnp.float32) + channel_sums).astype(jnp.bfloat16)


LANES = 128


def cost(flops, moved):
    return pl.CostEstimate(flops=flops, bytes_accessed=moved, transcendentals=0)


def slot(shift, size):
    wide = jnp.int32(shift) % size
    return jnp.where(wide < 0, wide + size, wide)


def project_kernel(scalars, *refs, size, extra_rank):
    chunks = refs[:size]
    gain = refs[size]
    outs = refs[-size - 1 : -1]
    scratch = refs[-1]
    weights = refs[size + 1 : -size - 1]
    extra = weights[-1] if extra_rank else None
    weights = weights[:-1] if extra_rank else weights
    width = sum(weight.shape[1] for weight in weights)
    rows = chunks[0].shape[0]
    lane = lax.broadcasted_iota(jnp.int32, (rows, LANES), 1)
    for index, chunk in enumerate(chunks):
        values = chunk[...].astype(jnp.float32)
        total = jnp.sum(values * values, axis=1, keepdims=True)
        scaled = (values * gain[...]).astype(jnp.bfloat16)
        if extra_rank:
            side = product(scaled, extra[...])
        else:
            side = jnp.zeros((rows, LANES), jnp.float32)
        high = total.astype(jnp.bfloat16).astype(jnp.float32)
        side = jnp.where(lane == extra_rank, high, side)
        side = jnp.where(lane == extra_rank + 1, total - high, side)
        scratch[scalars[index], :, : values.shape[1]] = scaled
        scratch[scalars[index], :, values.shape[1] :] = side.astype(jnp.bfloat16)
    inner = chunks[0].shape[1]
    for index, out in enumerate(outs):
        left = scratch[index, :, :inner]
        start = 0
        for weight in weights:
            stop = start + weight.shape[1]
            out[:, start:stop] = product(left, weight[...]).astype(jnp.bfloat16)
            start = stop
        out[:, width:] = scratch[index, :, inner:]


def project(chunks, order, gain, weights, extra, extra_rank):
    size = len(chunks)
    rows, inner = chunks[0].shape
    width = sum(weight.shape[1] for weight in weights) + LANES
    operands = [*chunks, gain.reshape(1, -1), *weights] + ([extra] if extra_rank else [])
    return pl.pallas_call(
        functools.partial(project_kernel, size=size, extra_rank=extra_rank),
        out_shape=[jax.ShapeDtypeStruct((rows, width), jnp.bfloat16)] * size,
        in_specs=[pl.BlockSpec(memory_space=pltpu.SMEM)]
        + [pl.BlockSpec(memory_space=pltpu.VMEM)] * len(operands),
        out_specs=[pl.BlockSpec(memory_space=pltpu.VMEM)] * size,
        scratch_shapes=[pltpu.VMEM((size, rows, inner + LANES), jnp.bfloat16)],
        cost_estimate=cost(2 * size * rows * inner * width, 2 * inner * width),
        name="project",
    )(order, *operands)


def spread_kernel(scalars, *refs, size):
    chunks = refs[:size]
    weight = refs[size]
    outs = refs[size + 1 : -1]
    scratch = refs[-1]
    for index, chunk in enumerate(chunks):
        scratch[scalars[index]] = chunk[...]
    for index, out in enumerate(outs):
        out[...] = product(scratch[index], weight[...]).astype(jnp.bfloat16)


def spread(chunks, order, weight):
    size = len(chunks)
    rows, inner = chunks[0].shape
    width = weight.shape[1]
    return pl.pallas_call(
        functools.partial(spread_kernel, size=size),
        out_shape=[jax.ShapeDtypeStruct((rows, width), jnp.bfloat16)] * size,
        in_specs=[pl.BlockSpec(memory_space=pltpu.SMEM)]
        + [pl.BlockSpec(memory_space=pltpu.VMEM)] * (size + 1),
        out_specs=[pl.BlockSpec(memory_space=pltpu.VMEM)] * size,
        scratch_shapes=[pltpu.VMEM((size, rows, inner), jnp.bfloat16)],
        cost_estimate=cost(2 * size * rows * inner * width, 2 * inner * width),
        name="spread",
    )(order, *chunks, weight)


def total_of(terms, start, stop):
    total = terms[0][:, start:stop].astype(jnp.float32)
    for term in terms[1:]:
        total = total + term[:, start:stop].astype(jnp.float32)
    return total


def inverse_root(side, extra_rank, features):
    squares = side[:, extra_rank : extra_rank + 1] + side[:, extra_rank + 1 : extra_rank + 2]
    return lax.rsqrt(squares / features + EPS)


def exact(left, right, dims):
    return lax.dot_general(
        left, right, (dims, ((), ())), precision=HIGH, preferred_element_type=jnp.float32
    )


def attend_kernel(*refs, size, key_cols, value_cols, rank, features):
    terms = refs[:size]
    decay_up, decay_bias, head_gain, out, attended_ref = refs[size:]
    width = 2 * key_cols + 2 * value_cols
    side = total_of(terms, width, width + LANES)
    scale = inverse_root(side, rank, features)
    lane = lax.broadcasted_iota(jnp.int32, side.shape, 1)
    low = jnp.where(lane < rank, side * scale, 0.0).astype(jnp.bfloat16)
    decay = jax.nn.log_sigmoid(product(low, decay_up[...]) + decay_bias[...]) / GATE_NORM
    length = side.shape[0]
    row = lax.broadcasted_iota(jnp.int32, (BLOCK, BLOCK), 0)
    column = lax.broadcasted_iota(jnp.int32, (BLOCK, BLOCK), 1)
    causal = row >= column
    lower = jnp.where(causal, 1.0, 0.0)

    def piece(start, stop):
        rounded = (total_of(terms, start, stop) * scale).astype(jnp.bfloat16)
        return rounded.astype(jnp.float32)

    queries = piece(0, key_cols) * DK ** (-0.5)
    key_rows = piece(key_cols, 2 * key_cols)
    value_rows = piece(2 * key_cols, 2 * key_cols + value_cols)
    gates = piece(2 * key_cols + value_cols, width)
    gates = gates / (1.0 + jnp.exp(-gates))
    for head in range(key_cols // DK):
        keys = slice(head * DK, (head + 1) * DK)
        values = slice(head * DV, (head + 1) * DV)
        state = None
        for block in range(length // BLOCK):
            here = slice(block * BLOCK, (block + 1) * BLOCK)
            running = exact(lower, decay[here, keys], ((1,), (0,)))
            final = running[BLOCK - 1 : BLOCK]
            query_in = queries[here, keys] * jnp.exp(running)
            keyed = key_rows[here, keys]
            valued = value_rows[here, values]
            scores = exact(query_in, keyed * jnp.exp(-running), ((1,), (1,)))
            scores = jnp.where(causal, scores, 0.0)
            attended = exact(scores, valued, ((1,), (0,)))
            if state is not None:
                attended = attended + exact(query_in, state, ((1,), (0,)))
            attended_ref[here, values] = attended
            if block + 1 < length // BLOCK:
                key_end = keyed * jnp.exp(final - running)
                update = exact(key_end, valued, ((0,), (0,)))
                factor = jnp.exp(final).reshape(DK, 1)
                state = update if state is None else factor * state + update
        heads = attended_ref[:, values]
        normed = root_norm(heads, head_gain[...])
        out[:, values] = (normed * gates[:, values]).astype(jnp.bfloat16)


def attend(terms, decay_up, decay_bias, head_gain, key_cols, value_cols, rank, features):
    rows = terms[0].shape[0]
    return pl.pallas_call(
        functools.partial(
            attend_kernel,
            size=len(terms),
            key_cols=key_cols,
            value_cols=value_cols,
            rank=rank,
            features=features,
        ),
        out_shape=jax.ShapeDtypeStruct((rows, value_cols), jnp.bfloat16),
        scratch_shapes=[pltpu.VMEM((rows, value_cols), jnp.float32)],
        name="attend",
    )(*terms, decay_up, decay_bias.reshape(1, -1), head_gain.reshape(1, -1))


def up_kernel(scalars, *refs, size, features):
    streams = refs[: size * size]
    mine = refs[size * size : size * size + size]
    other = refs[size * size + size : size * size + 2 * size]
    gain, taps_gate, taps_value, out, scratch = refs[size * size + 2 * size :]
    rows, inner = streams[0].shape
    width = out.shape[1]
    first = scalars[size] == 0
    position = lax.broadcasted_iota(jnp.int32, (rows, width), 0)

    def conv(values, taps):
        values = values.astype(jnp.bfloat16).astype(jnp.float32)
        total = jnp.zeros_like(values)
        for offset in range(CONV):
            back = CONV - 1 - offset
            moved = pltpu.roll(values, back, 0) if back else values
            moved = jnp.where(position >= back, moved, 0.0)
            total = total + moved * taps[offset : offset + 1]
        return total

    for index in range(size):
        here = streams[index * size : (index + 1) * size]
        squares = jnp.zeros((rows, 1), jnp.float32)
        for chunk in here:
            values = chunk[...].astype(jnp.float32)
            squares = squares + jnp.sum(values * values, axis=1, keepdims=True)
        scale = lax.rsqrt(squares / features + EPS)
        for block, chunk in enumerate(here):
            values = chunk[...].astype(jnp.float32) * scale * gain[scalars[block]]
            scratch[
                index * rows : (index + 1) * rows, block * inner : (block + 1) * inner
            ] = values.astype(jnp.bfloat16)
    left = jnp.zeros((size * rows, width), jnp.float32)
    right = jnp.zeros((size * rows, width), jnp.float32)
    for block in range(size):
        piece = scratch[:, block * inner : (block + 1) * inner]
        left = left + product(piece, mine[block][...])
        right = right + product(piece, other[block][...])
    for index in range(size):
        cut = slice(index * rows, (index + 1) * rows)
        gates = conv(jnp.where(first, left[cut], right[cut]), taps_gate)
        values = conv(jnp.where(first, right[cut], left[cut]), taps_value)
        out[cut] = (jax.nn.gelu(gates, approximate=True) * values).astype(jnp.bfloat16)


def up_units(scalars, streams, mine, other, gain, taps_gate, taps_value, features):
    size = len(mine)
    rows, inner = streams[0].shape
    width = taps_gate.shape[1]
    operands = [*streams, *mine, *other, gain.reshape(size, 1, inner), taps_gate, taps_value]
    return pl.pallas_call(
        functools.partial(up_kernel, size=size, features=features),
        out_shape=jax.ShapeDtypeStruct((size * rows, width), jnp.bfloat16),
        in_specs=[pl.BlockSpec(memory_space=pltpu.SMEM)]
        + [pl.BlockSpec(memory_space=pltpu.VMEM)] * len(operands),
        out_specs=pl.BlockSpec(memory_space=pltpu.VMEM),
        scratch_shapes=[pltpu.VMEM((size * rows, features), jnp.bfloat16)],
        cost_estimate=cost(4 * size * rows * features * width, 4 * features * width),
        name="up",
    )(scalars, *operands)


def down_kernel(scalars, *refs, size):
    chunks = refs[:size]
    weight = refs[size]
    outs = refs[size + 1 :]
    width = chunks[0].shape[1]
    rows = outs[0].shape[0]
    total = jnp.zeros((chunks[0].shape[0], weight.shape[1]), jnp.float32)
    for block, chunk in enumerate(chunks):
        start = pl.multiple_of(scalars[block] * width, width)
        total = total + product(chunk[...], weight[pl.ds(start, width)])
    for index, out in enumerate(outs):
        out[...] = total[index * rows : (index + 1) * rows].astype(jnp.bfloat16)


def down_terms(scalars, chunks, weight):
    size = len(chunks)
    rows = chunks[0].shape[0] // size
    width = weight.shape[1]
    return pl.pallas_call(
        functools.partial(down_kernel, size=size),
        out_shape=[jax.ShapeDtypeStruct((rows, width), jnp.bfloat16)] * size,
        in_specs=[pl.BlockSpec(memory_space=pltpu.SMEM)]
        + [pl.BlockSpec(memory_space=pltpu.VMEM)] * (size + 1),
        out_specs=[pl.BlockSpec(memory_space=pltpu.VMEM)] * size,
        cost_estimate=cost(2 * size * rows * weight.shape[0] * width, 2 * weight.size),
        name="down",
    )(scalars, *chunks, weight)


def moving_activations(
    inputs,
    mix_gain,
    query_weight,
    key_weight,
    value_weight,
    outgate_weight,
    decay_down,
    decay_up,
    decay_bias,
    head_gain,
    mixout_weight,
    ffn_gain,
    upgate_weight,
    upvalue_weight,
    conv_gate,
    conv_value,
    down_weight,
    *,
    size,
):
    line = lax.axis_index("fs")
    position = lax.axis_index("tp")
    features = mix_gain.shape[0]
    own = query_weight.shape[0]
    key_cols = query_weight.shape[1]
    value_cols = value_weight.shape[1]
    hidden_cols = upgate_weight.shape[1]
    rank = decay_down.shape[1]
    steps = range(size)
    both = ("fs", "tp")

    def along(axis, shift, array):
        if shift == 0:
            return array
        return lax.ppermute(array, axis, [(at, (at + shift) % size) for at in steps])

    def across(mask, array):
        if mask == 0:
            return array
        return lax.ppermute(array, "tp", [(at, at ^ mask) for at in steps])

    def spread_along(array):
        found = [array]
        span = size // 2
        masks = [0]
        while span:
            found = found + [across(span, item) for item in found]
            masks = masks + [mask ^ span for mask in masks]
            span //= 2
        return [found[masks.index(mask)] for mask in steps]

    def crossed(array):
        pairs = [(a * size + b, b * size + a) for a in steps for b in steps]
        return lax.ppermute(array, both, pairs)

    def summed(terms):
        total = terms[0].astype(jnp.float32)
        for term in terms[1:]:
            total = total + term.astype(jnp.float32)
        return total

    own_gain = lax.dynamic_slice_in_dim(mix_gain, line * own, own, 0)
    own_down = lax.dynamic_slice_in_dim(decay_down, line * own, own, 0)
    own_down = jnp.pad(own_down, ((0, 0), (0, LANES - rank)))
    own_up = lax.dynamic_slice_in_dim(decay_up, position * key_cols, key_cols, 1)
    own_up = jnp.pad(own_up, ((0, LANES - rank), (0, 0)))
    own_bias = lax.dynamic_slice_in_dim(decay_bias, position * key_cols, key_cols, 0)
    part = hidden_cols // size
    taps_at = position * hidden_cols + line * part
    taps_gate = lax.dynamic_slice_in_dim(conv_gate, taps_at, part, 1)
    taps_value = lax.dynamic_slice_in_dim(conv_value, taps_at, part, 1)
    group = lax.axis_index("grp")

    turned = crossed(inputs)

    turned, first_up, second_up = lax.optimization_barrier((turned, upgate_weight, upvalue_weight))
    fetched = jnp.where(group == 0, first_up, second_up)
    untouched = jnp.where(group == 0, second_up, first_up)

    def units(array, shift):
        return lax.dynamic_slice_in_dim(array, slot(line + shift, size) * part, part, 1)

    mine = [along("fs", shift, units(fetched, shift)) for shift in steps]
    other = [units(untouched, 0)]
    other += [lax.ppermute(item, "grp", [(0, 1), (1, 0)]) for item in mine[1:]]

    chunks = spread_along(turned)
    parts = project(
        chunks,
        jnp.stack([slot((position ^ mask) - line, size) for mask in steps]),
        own_gain,
        (query_weight, key_weight, value_weight, outgate_weight),
        own_down,
        rank,
    )
    terms = [along("fs", shift, parts[shift]) for shift in steps]
    gated = attend(terms, own_up, own_bias, head_gain, key_cols, value_cols, rank, features)

    before = [slot(line - shift, size) for shift in steps]
    rows = [along("fs", shift, gated) for shift in steps]
    parts = spread(rows, jnp.stack([position ^ index for index in before]), mixout_weight)
    mixed = summed([across(mask, parts[mask]) for mask in steps])
    stream = (turned.astype(jnp.float32) + mixed).astype(jnp.bfloat16)
    blocks = [spread_along(along("fs", shift, stream)) for shift in steps]
    streams = [blocks[shift][mask] for mask in steps for shift in steps]
    hidden = up_units(
        jnp.stack(before + [group]), streams, mine, other, ffn_gain, taps_gate, taps_value, features
    )

    rows = [along("fs", shift, hidden) for shift in steps]
    parts = down_terms(jnp.stack(before), rows, down_weight)
    channel_sums = summed([across(mask, parts[mask]) for mask in steps])
    return crossed((stream.astype(jnp.float32) + channel_sums).astype(jnp.bfloat16))


def solution(mesh):
    plan = per_device
    size = mesh.shape["fs"]
    if size == mesh.shape["tp"] and size & (size - 1) == 0 and mesh.shape["grp"] == 2:
        plan = functools.partial(moving_activations, size=size)
    return jax.shard_map(
        plan,
        mesh=mesh,
        in_specs=(
            P(("grp", "fs"), "tp"),
            P(),
            P("fs", "tp"),
            P("fs", "tp"),
            P("fs", "tp"),
            P("fs", "tp"),
            P(),
            P(),
            P(),
            P(),
            P("tp", "fs"),
            P(),
            P("fs", "tp"),
            P("fs", "tp"),
            P(),
            P(),
            P("tp", "fs"),
        ),
        out_specs=P(("grp", "fs"), "tp"),
        check_vma=False,
    )
```

```python
import functools

import jax
import jax.numpy as jnp
from jax import lax
from jax.experimental import pallas as pl
from jax.experimental.pallas import tpu as pltpu
from jax.sharding import PartitionSpec as P

DK = 128
DV = 256
BLOCK = 64
CONV = 3


EPS = 1e-06
GATE_NORM = 16.0
HIGH = lax.Precision.HIGHEST


def product(left, right):
    return jnp.dot(left, right, preferred_element_type=jnp.float32)


def root_norm(values, gain):
    return values * lax.rsqrt(jnp.mean(values * values, axis=-1, keepdims=True) + EPS) * gain


def linear_attention(queries, key_rows, value_rows, log_decay):
    count, length, heads, key_size = queries.shape
    blocks = length // BLOCK

    def split(tensor):
        return (
            tensor.astype(jnp.float32)
            .reshape(count, blocks, BLOCK, heads, -1)
            .transpose(0, 3, 1, 2, 4)
        )

    scaled = split(queries) * key_size ** (-0.5)
    keyed = split(key_rows)
    valued = split(value_rows)
    running = jnp.cumsum(split(log_decay), axis=3)
    final = running[:, :, :, -1:]
    query_in = scaled * jnp.exp(running)
    key_in = keyed * jnp.exp(-running)
    key_end = keyed * jnp.exp(final - running)
    causal = jnp.tril(jnp.ones((BLOCK, BLOCK), dtype=bool))
    scores = jnp.einsum("shnik,shnjk->shnij", query_in, key_in, precision=HIGH)
    scores = jnp.where(causal, scores, 0.0)
    inside = jnp.einsum("shnij,shnjv->shniv", scores, valued, precision=HIGH)
    update = jnp.einsum("shnck,shncv->shnkv", key_end, valued, precision=HIGH)
    factor = jnp.exp(final[:, :, :, 0])

    def advance(state, pair):
        return (pair[0][..., None] * state + pair[1], state)

    initial = jnp.zeros((count, heads, key_size, valued.shape[-1]), jnp.float32)
    _, starts = lax.scan(advance, initial, (jnp.moveaxis(factor, 2, 0), jnp.moveaxis(update, 2, 0)))
    starts = jnp.moveaxis(starts, 0, 2)
    carried = jnp.einsum("shnck,shnkv->shncv", query_in, starts, precision=HIGH)
    merged = inside + carried
    return merged.transpose(0, 2, 3, 1, 4).reshape(count, length, heads * valued.shape[-1])


def causal_conv(rows, taps):
    length = rows.shape[0]
    padded = jnp.pad(rows.astype(jnp.float32), ((CONV - 1, 0), (0, 0)))
    total = jnp.zeros((length, rows.shape[1]), jnp.float32)
    for offset in range(CONV):
        total = total + padded[offset : offset + length] * taps[offset]
    return total


def per_device(
    inputs,
    mix_gain,
    query_weight,
    key_weight,
    value_weight,
    outgate_weight,
    decay_down,
    decay_up,
    decay_bias,
    head_gain,
    mixout_weight,
    ffn_gain,
    upgate_weight,
    upvalue_weight,
    conv_gate,
    conv_value,
    down_weight,
):
    position = lax.axis_index("tp")
    whole = lax.all_gather(inputs, "tp", axis=1, tiled=True)
    normed_mix = root_norm(whole.astype(jnp.float32), mix_gain).astype(jnp.bfloat16)
    length = normed_mix.shape[0]
    key_cols = query_weight.shape[1]
    value_cols = value_weight.shape[1]
    local_heads = key_cols // DK
    pieces = (
        lax.all_gather(query_weight, "fs", axis=0, tiled=True),
        lax.all_gather(key_weight, "fs", axis=0, tiled=True),
        lax.all_gather(value_weight, "fs", axis=0, tiled=True),
        lax.all_gather(outgate_weight, "fs", axis=0, tiled=True),
    )
    queries, key_rows, value_rows, out_gates = tuple(
        (product(normed_mix, piece) for piece in pieces)
    )
    queries = queries.astype(jnp.bfloat16)
    key_rows = key_rows.astype(jnp.bfloat16)
    value_rows = value_rows.astype(jnp.bfloat16)
    out_gates = out_gates.astype(jnp.bfloat16)
    decay_low = product(normed_mix, decay_down).astype(jnp.bfloat16)
    own_up = lax.dynamic_slice_in_dim(decay_up, position * key_cols, key_cols, 1)
    own_bias = lax.dynamic_slice_in_dim(decay_bias, position * key_cols, key_cols, 0)
    log_decay = jax.nn.log_sigmoid(product(decay_low, own_up) + own_bias) / GATE_NORM
    attended = linear_attention(
        queries.reshape(1, length, local_heads, DK),
        key_rows.reshape(1, length, local_heads, DK),
        value_rows.reshape(1, length, local_heads, DV),
        log_decay.reshape(1, length, local_heads, DK),
    )
    attended = attended.reshape(length, local_heads, DV)
    gated = root_norm(attended, head_gain) * jax.nn.silu(
        out_gates.astype(jnp.float32).reshape(length, local_heads, DV)
    )
    gated = gated.reshape(length, value_cols).astype(jnp.bfloat16)
    mix_terms = product(gated, lax.all_gather(mixout_weight, "fs", axis=1, tiled=True))
    mixed = lax.psum_scatter(
        mix_terms.astype(jnp.bfloat16), "tp", scatter_dimension=1, tiled=True
    ).astype(jnp.float32)
    stream = (inputs.astype(jnp.float32) + mixed).astype(jnp.bfloat16)
    whole_stream = lax.all_gather(stream, "tp", axis=1, tiled=True)
    normed_ffn = root_norm(whole_stream.astype(jnp.float32), ffn_gain).astype(jnp.bfloat16)
    hidden_cols = upgate_weight.shape[1]
    gate_full, value_full = (
        lax.all_gather(upgate_weight, "fs", axis=0, tiled=True),
        lax.all_gather(upvalue_weight, "fs", axis=0, tiled=True),
    )
    up_gates = product(normed_ffn, gate_full)
    up_values = product(normed_ffn, value_full)
    up_gates = up_gates.astype(jnp.bfloat16)
    up_values = up_values.astype(jnp.bfloat16)
    taps_gate = lax.dynamic_slice_in_dim(conv_gate, position * hidden_cols, hidden_cols, 1)
    taps_value = lax.dynamic_slice_in_dim(conv_value, position * hidden_cols, hidden_cols, 1)
    conv_gates = causal_conv(up_gates, taps_gate)
    conv_values = causal_conv(up_values, taps_value)
    hidden = (jax.nn.gelu(conv_gates, approximate=True) * conv_values).astype(jnp.bfloat16)
    down_terms = product(hidden, lax.all_gather(down_weight, "fs", axis=1, tiled=True))
    channel_sums = lax.psum_scatter(
        down_terms.astype(jnp.bfloat16), "tp", scatter_dimension=1, tiled=True
    ).astype(jnp.float32)
    return (stream.astype(jnp.float32) + channel_sums).astype(jnp.bfloat16)


LANES = 128


def cost(flops, moved):
    return pl.CostEstimate(flops=flops, bytes_accessed=moved, transcendentals=0)


def slot(shift, size):
    wide = jnp.int32(shift) % size
    return jnp.where(wide < 0, wide + size, wide)


def project_kernel(scalars, *refs, size, waited, paired):
    refs = refs[waited:]
    chunks = refs[:size]
    outs = refs[-size - 1 : -1]
    scratch = refs[-1]
    weights = refs[size : -size - 2]
    extra = refs[-size - 2]
    width = sum(weight.shape[1] for weight in weights)
    for index, chunk in enumerate(chunks):
        scratch[scalars[index]] = chunk[...]
    for index, out in enumerate(outs):
        left = scratch[index]
        start = 0
        for place, weight in enumerate(weights):
            stop = start + weight.shape[1]
            whole = product(left, weight[...])
            high = whole.astype(jnp.bfloat16)
            out[:, start:stop] = high
            if place < paired:
                rest = whole - high.astype(jnp.float32)
                out[:, width + start : width + stop] = rest.astype(jnp.bfloat16)
            start = stop
        out[:, -LANES:] = product(left, extra[...]).astype(jnp.bfloat16)


def project(chunks, order, weights, paired, extra, awaited):
    size = len(chunks)
    rows, inner = chunks[0].shape
    width = sum(weight.shape[1] for weight in weights) + LANES
    width += sum(weight.shape[1] for weight in weights[:paired])
    operands = [*chunks, *weights, extra]
    return pl.pallas_call(
        functools.partial(
            project_kernel, size=size, waited=len(awaited), paired=paired
        ),
        out_shape=[jax.ShapeDtypeStruct((rows, width), jnp.bfloat16)] * size,
        in_specs=[pl.BlockSpec(memory_space=pltpu.SMEM)]
        + [pl.BlockSpec(memory_space=pl.ANY)] * len(awaited)
        + [pl.BlockSpec(memory_space=pltpu.VMEM)] * len(operands),
        out_specs=[pl.BlockSpec(memory_space=pltpu.VMEM)] * size,
        scratch_shapes=[pltpu.VMEM((size, rows, inner), jnp.bfloat16)],
        cost_estimate=cost(2 * size * rows * inner * width, 2 * inner * width),
        name="project",
    )(order, *awaited, *operands)


def spread_kernel(scalars, *refs, size):
    chunks = refs[:size]
    weight = refs[size]
    outs = refs[size + 1 : -1]
    scratch = refs[-1]
    for index, chunk in enumerate(chunks):
        scratch[scalars[index]] = chunk[...]
    for index, out in enumerate(outs):
        out[...] = product(scratch[index], weight[...]).astype(jnp.bfloat16)


def spread(chunks, order, weight):
    size = len(chunks)
    rows, inner = chunks[0].shape
    width = weight.shape[1]
    return pl.pallas_call(
        functools.partial(spread_kernel, size=size),
        out_shape=[jax.ShapeDtypeStruct((rows, width), jnp.bfloat16)] * size,
        in_specs=[pl.BlockSpec(memory_space=pltpu.SMEM)]
        + [pl.BlockSpec(memory_space=pltpu.VMEM)] * (size + 1),
        out_specs=[pl.BlockSpec(memory_space=pltpu.VMEM)] * size,
        scratch_shapes=[pltpu.VMEM((size, rows, inner), jnp.bfloat16)],
        cost_estimate=cost(2 * size * rows * inner * width, 2 * inner * width),
        name="spread",
    )(order, *chunks, weight)


def total_of(terms, start, stop):
    total = terms[0][:, start:stop].astype(jnp.float32)
    for term in terms[1:]:
        total = total + term[:, start:stop].astype(jnp.float32)
    return total


def exact(left, right, dims):
    return lax.dot_general(
        left, right, (dims, ((), ())), precision=HIGH, preferred_element_type=jnp.float32
    )


def attend_kernel(*refs, size, key_cols, value_cols, waited):
    refs = refs[waited:]
    terms = refs[:size]
    decay_up, decay_bias, head_gain, out, attended_ref = refs[size:]
    width = 2 * key_cols + 2 * value_cols
    side = total_of(terms, width + 2 * key_cols, width + 2 * key_cols + LANES)
    low = side.astype(jnp.bfloat16)
    decay = jax.nn.log_sigmoid(product(low, decay_up[...]) + decay_bias[...]) / GATE_NORM
    length = side.shape[0]
    row = lax.broadcasted_iota(jnp.int32, (BLOCK, BLOCK), 0)
    column = lax.broadcasted_iota(jnp.int32, (BLOCK, BLOCK), 1)
    causal = row >= column
    lower = jnp.where(causal, 1.0, 0.0)

    def piece(start, stop, paired=False):
        total = total_of(terms, start, stop)
        if paired:
            total = total + total_of(terms, width + start, width + stop)
        return total.astype(jnp.bfloat16).astype(jnp.float32)

    queries = piece(0, key_cols, True) * DK ** (-0.5)
    key_rows = piece(key_cols, 2 * key_cols, True)
    value_rows = piece(2 * key_cols, 2 * key_cols + value_cols)
    gates = piece(2 * key_cols + value_cols, width)
    gates = gates / (1.0 + jnp.exp(-gates))
    for head in range(key_cols // DK):
        keys = slice(head * DK, (head + 1) * DK)
        values = slice(head * DV, (head + 1) * DV)
        state = None
        for block in range(length // BLOCK):
            here = slice(block * BLOCK, (block + 1) * BLOCK)
            running = exact(lower, decay[here, keys], ((1,), (0,)))
            final = running[BLOCK - 1 : BLOCK]
            query_in = queries[here, keys] * jnp.exp(running)
            keyed = key_rows[here, keys]
            valued = value_rows[here, values]
            scores = exact(query_in, keyed * jnp.exp(-running), ((1,), (1,)))
            scores = jnp.where(causal, scores, 0.0)
            attended = exact(scores, valued, ((1,), (0,)))
            if state is not None:
                attended = attended + exact(query_in, state, ((1,), (0,)))
            attended_ref[here, values] = attended
            if block + 1 < length // BLOCK:
                key_end = keyed * jnp.exp(final - running)
                update = exact(key_end, valued, ((0,), (0,)))
                factor = jnp.exp(final).reshape(DK, 1)
                state = update if state is None else factor * state + update
        heads = attended_ref[:, values]
        normed = root_norm(heads, head_gain[...])
        out[:, values] = (normed * gates[:, values]).astype(jnp.bfloat16)


def attend(
    terms, decay_up, decay_bias, head_gain, key_cols, value_cols, awaited
):
    rows = terms[0].shape[0]
    return pl.pallas_call(
        functools.partial(
            attend_kernel,
            size=len(terms),
            key_cols=key_cols,
            value_cols=value_cols,
            waited=len(awaited),
        ),
        out_shape=jax.ShapeDtypeStruct((rows, value_cols), jnp.bfloat16),
        in_specs=[pl.BlockSpec(memory_space=pl.ANY)] * len(awaited)
        + [pl.BlockSpec(memory_space=pltpu.VMEM)] * (len(terms) + 3),
        scratch_shapes=[pltpu.VMEM((rows, value_cols), jnp.float32)],
        name="attend",
    )(*awaited, *terms, decay_up, decay_bias.reshape(1, -1), head_gain.reshape(1, -1))


def up_kernel(scalars, *refs, size, features):
    streams = refs[: size * size]
    mine = refs[size * size : size * size + size]
    other = refs[size * size + size : size * size + 2 * size]
    gain, taps_gate, taps_value, out, scratch = refs[size * size + 2 * size :]
    rows, inner = streams[0].shape
    width = out.shape[1]
    first = scalars[size] == 0
    position = lax.broadcasted_iota(jnp.int32, (rows, width), 0)

    def conv(values, taps):
        values = values.astype(jnp.bfloat16).astype(jnp.float32)
        total = jnp.zeros_like(values)
        for offset in range(CONV):
            back = CONV - 1 - offset
            moved = pltpu.roll(values, back, 0) if back else values
            moved = jnp.where(position >= back, moved, 0.0)
            total = total + moved * taps[offset : offset + 1]
        return total

    for index in range(size):
        here = streams[index * size : (index + 1) * size]
        squares = jnp.zeros((rows, 1), jnp.float32)
        for chunk in here:
            values = chunk[...].astype(jnp.float32)
            squares = squares + jnp.sum(values * values, axis=1, keepdims=True)
        scale = lax.rsqrt(squares / features + EPS)
        for block, chunk in enumerate(here):
            values = chunk[...].astype(jnp.float32) * scale * gain[scalars[block]]
            scratch[
                index * rows : (index + 1) * rows, block * inner : (block + 1) * inner
            ] = values.astype(jnp.bfloat16)
    left = jnp.zeros((size * rows, width), jnp.float32)
    right = jnp.zeros((size * rows, width), jnp.float32)
    for block in range(size):
        piece = scratch[:, block * inner : (block + 1) * inner]
        left = left + product(piece, mine[block][...])
        right = right + product(piece, other[block][...])
    for index in range(size):
        cut = slice(index * rows, (index + 1) * rows)
        gates = conv(jnp.where(first, left[cut], right[cut]), taps_gate)
        values = conv(jnp.where(first, right[cut], left[cut]), taps_value)
        out[cut] = (jax.nn.gelu(gates, approximate=True) * values).astype(jnp.bfloat16)


def up_units(scalars, streams, mine, other, gain, taps_gate, taps_value, features):
    size = len(mine)
    rows, inner = streams[0].shape
    width = taps_gate.shape[1]
    operands = [*streams, *mine, *other, gain.reshape(size, 1, inner), taps_gate, taps_value]
    return pl.pallas_call(
        functools.partial(up_kernel, size=size, features=features),
        out_shape=jax.ShapeDtypeStruct((size * rows, width), jnp.bfloat16),
        in_specs=[pl.BlockSpec(memory_space=pltpu.SMEM)]
        + [pl.BlockSpec(memory_space=pltpu.VMEM)] * len(operands),
        out_specs=pl.BlockSpec(memory_space=pltpu.VMEM),
        scratch_shapes=[pltpu.VMEM((size * rows, features), jnp.bfloat16)],
        cost_estimate=cost(4 * size * rows * features * width, 4 * features * width),
        name="up",
    )(scalars, *operands)


def down_kernel(scalars, *refs, size):
    chunks = refs[:size]
    weight = refs[size]
    outs = refs[size + 1 :]
    width = chunks[0].shape[1]
    rows = outs[0].shape[0]
    total = jnp.zeros((chunks[0].shape[0], weight.shape[1]), jnp.float32)
    for block, chunk in enumerate(chunks):
        start = pl.multiple_of(scalars[block] * width, width)
        total = total + product(chunk[...], weight[pl.ds(start, width)])
    for index, out in enumerate(outs):
        out[...] = total[index * rows : (index + 1) * rows].astype(jnp.bfloat16)


def down_terms(scalars, chunks, weight):
    size = len(chunks)
    rows = chunks[0].shape[0] // size
    width = weight.shape[1]
    return pl.pallas_call(
        functools.partial(down_kernel, size=size),
        out_shape=[jax.ShapeDtypeStruct((rows, width), jnp.bfloat16)] * size,
        in_specs=[pl.BlockSpec(memory_space=pltpu.SMEM)]
        + [pl.BlockSpec(memory_space=pltpu.VMEM)] * (size + 1),
        out_specs=[pl.BlockSpec(memory_space=pltpu.VMEM)] * size,
        cost_estimate=cost(2 * size * rows * weight.shape[0] * width, 2 * weight.size),
        name="down",
    )(scalars, *chunks, weight)


def moving_activations(
    inputs,
    mix_gain,
    query_weight,
    key_weight,
    value_weight,
    outgate_weight,
    decay_down,
    decay_up,
    decay_bias,
    head_gain,
    mixout_weight,
    ffn_gain,
    upgate_weight,
    upvalue_weight,
    conv_gate,
    conv_value,
    down_weight,
    *,
    size,
):
    line = lax.axis_index("fs")
    position = lax.axis_index("tp")
    features = mix_gain.shape[0]
    own = query_weight.shape[0]
    key_cols = query_weight.shape[1]
    value_cols = value_weight.shape[1]
    hidden_cols = upgate_weight.shape[1]
    rank = decay_down.shape[1]
    steps = range(size)
    both = ("fs", "tp")

    def along(axis, shift, array):
        if shift == 0:
            return array
        return lax.ppermute(array, axis, [(at, (at + shift) % size) for at in steps])

    def across(mask, array):
        if mask == 0:
            return array
        return lax.ppermute(array, "tp", [(at, at ^ mask) for at in steps])

    def spread_along(array):
        found = [array]
        span = size // 2
        masks = [0]
        while span:
            found = found + [across(span, item) for item in found]
            masks = masks + [mask ^ span for mask in masks]
            span //= 2
        return [found[masks.index(mask)] for mask in steps]

    def crossed(array):
        pairs = [(a * size + b, b * size + a) for a in steps for b in steps]
        return lax.ppermute(array, both, pairs)

    def summed(terms):
        total = terms[0].astype(jnp.float32)
        for term in terms[1:]:
            total = total + term.astype(jnp.float32)
        return total

    own_gain = lax.dynamic_slice_in_dim(mix_gain, line * own, own, 0)
    own_down = lax.dynamic_slice_in_dim(decay_down, line * own, own, 0)
    own_down = jnp.pad(own_down, ((0, 0), (0, LANES - rank)))
    own_up = lax.dynamic_slice_in_dim(decay_up, position * key_cols, key_cols, 1)
    own_up = jnp.pad(own_up, ((0, LANES - rank), (0, 0)))
    own_bias = lax.dynamic_slice_in_dim(decay_bias, position * key_cols, key_cols, 0)
    part = hidden_cols // size
    taps_at = position * hidden_cols + line * part
    taps_gate = lax.dynamic_slice_in_dim(conv_gate, taps_at, part, 1)
    taps_value = lax.dynamic_slice_in_dim(conv_value, taps_at, part, 1)
    group = lax.axis_index("grp")

    turned = crossed(inputs)

    fetched = jnp.where(group == 0, upgate_weight, upvalue_weight)
    untouched = jnp.where(group == 0, upvalue_weight, upgate_weight)

    def units(array, shift):
        return lax.dynamic_slice_in_dim(array, slot(line + shift, size) * part, part, 1)

    mine = [along("fs", shift, units(fetched, shift)) for shift in steps]
    other = [units(untouched, 0)]
    other += [lax.ppermute(item, "grp", [(0, 1), (1, 0)]) for item in mine[1:]]

    wide = turned.astype(jnp.float32)
    squares = jnp.sum(wide * wide, axis=1).reshape(1, -1)
    squares = summed([along("fs", shift, squares) for shift in steps]).reshape(-1, 1)
    normed = wide * lax.rsqrt(squares / features + EPS) * own_gain
    chunks = spread_along(normed.astype(jnp.bfloat16))
    parts = project(
        chunks,
        jnp.stack([slot((position ^ mask) - line, size) for mask in steps]),
        (query_weight, key_weight, value_weight, outgate_weight),
        2,
        own_down,
        mine[1:],
    )
    terms = [along("fs", shift, parts[shift]) for shift in steps]
    gated = attend(
        terms, own_up, own_bias, head_gain, key_cols, value_cols, other[1:]
    )

    before = [slot(line - shift, size) for shift in steps]
    rows = [along("fs", shift, gated) for shift in steps]
    parts = spread(rows, jnp.stack([position ^ index for index in before]), mixout_weight)
    mixed = summed([across(mask, parts[mask]) for mask in steps])
    stream = (turned.astype(jnp.float32) + mixed).astype(jnp.bfloat16)
    blocks = [spread_along(along("fs", shift, stream)) for shift in steps]
    streams = [blocks[shift][mask] for mask in steps for shift in steps]
    hidden = up_units(
        jnp.stack(before + [group]), streams, mine, other, ffn_gain, taps_gate, taps_value, features
    )

    rows = [along("fs", shift, hidden) for shift in steps]
    parts = down_terms(jnp.stack(before), rows, down_weight)
    channel_sums = summed([across(mask, parts[mask]) for mask in steps])
    return crossed((stream.astype(jnp.float32) + channel_sums).astype(jnp.bfloat16))


def solution(mesh):
    plan = per_device
    size = mesh.shape["fs"]
    if size == mesh.shape["tp"] and size & (size - 1) == 0 and mesh.shape["grp"] == 2:
        plan = functools.partial(moving_activations, size=size)
    return jax.shard_map(
        plan,
        mesh=mesh,
        in_specs=(
            P(("grp", "fs"), "tp"),
            P(),
            P("fs", "tp"),
            P("fs", "tp"),
            P("fs", "tp"),
            P("fs", "tp"),
            P(),
            P(),
            P(),
            P(),
            P("tp", "fs"),
            P(),
            P("fs", "tp"),
            P("fs", "tp"),
            P(),
            P(),
            P("tp", "fs"),
        ),
        out_specs=P(("grp", "fs"), "tp"),
        check_vma=False,
    )
```
